32 devices in a mesh: sp: 4 (over y, core), dp: 8 (over z, x).
Axes of the slice: x: 2, y: 2, z: 4, core: 2. Of those that a mesh axis runs over, the one named last changes fastest.
Arguments:
- q_latent: bfloat16 [8, 512, 512], P('dp', 'sp'), may hold values from -70 to 70
- kv_latent: bfloat16 [8, 512, 512], P('dp', 'sp'), may hold values from -70 to 70
- rope_key: bfloat16 [8, 512, 64], P('dp', 'sp'), may hold values from -370 to 370
- w_query: bfloat16 [512, 3072], P(None, 'dp'), may hold values from -0.25 to 0.25
- w_keyval: bfloat16 [512, 4096], P(None, 'sp'), may hold values from -0.25 to 0.25
- w_out: bfloat16 [2048, 2048], replicated, may hold values from -0.125 to 0.125
- query_gain: bfloat16 [512], replicated, may hold values from 0.099609375 to 1.8984375
- latent_gain: bfloat16 [512], replicated, may hold values from 0.099609375 to 1.8984375
- out_gain: bfloat16 [2048], replicated, may hold values from 0.099609375 to 1.8984375
Outputs:
- output: bfloat16 [8, 512, 2048], P('dp', 'sp')
The draws below stay inside these ranges and needn't reach their ends.
All inputs are finite; a program needn't handle non-finite values.
Results may differ from the reference program's by a relative error of at most 0.03.
The reference program's roundings to bfloat16 on the way (of `query_norm`, `queries`, `latent_norm`, `keyval`, `rope_turned`, `weights`, `attended` and `mixed_norm`) count: a program that leaves them out, or rounds other values in their place, can miss the bound.
Values may be sent and summed in bfloat16 or wider, within the bound.
No kernel may reach another device: no remote copies, remote signals or barrier semaphores. Data moves between devices by JAX's collectives and lax.ppermute only.
A program may use at most 64 MiB of HBM per device.

```python
import math
import jax
import jax.numpy as jnp
from jax import lax

D = 2048
H = 16
QR = 512
KR = 512
NOPE = 128
ROPE = 64
VDIM = 128
SEQ_LEN = 512
SEQS = 8


def scaled_latent_draw(key, width):
    base_key, channel_key, row_key = jax.random.split(key, 3)
    array_shape = (SEQS, SEQ_LEN, width)
    base_draw = jnp.clip(jax.random.normal(base_key, array_shape, jnp.float32), -5.0, 5.0)
    channel = jnp.exp(jax.random.uniform(channel_key, (width,), jnp.float32, math.log(0.3), math.log(3.0)))
    row_scale = jnp.exp(jax.random.uniform(row_key, (SEQS, SEQ_LEN, 1), jnp.float32, math.log(0.3), math.log(3.0)))
    return base_draw * channel * row_scale


def draw_q_latent(key, part):
    return scaled_latent_draw(jax.random.fold_in(key, 11), QR).astype(jnp.bfloat16)


def draw_kv_latent(key, part):
    return scaled_latent_draw(jax.random.fold_in(key, 12), KR).astype(jnp.bfloat16)


def draw_rope_key(key, part):
    base_key = jax.random.fold_in(jax.random.fold_in(key, 13), 0)
    array_shape = (SEQS, SEQ_LEN, ROPE)
    result_draw = jnp.clip(jax.random.normal(base_key, array_shape, jnp.float32), -5.0, 5.0)
    return result_draw.astype(jnp.bfloat16)


def steps_of(own_key, extent, cuts, least, largest):
    gain = 1.0
    for dim, parts in cuts:
        draws = jax.random.uniform(jax.random.fold_in(jax.random.fold_in(own_key, 6), dim), (parts,), jnp.float32, least / len(cuts), largest / len(cuts))
        gain = gain * jnp.repeat(jnp.exp(draws), extent[dim] // parts).reshape((-1,) + (1,) * (len(extent) - 1 - dim))
    return gain


def noise(own_key, shape, scale, limit, cuts=(), kind=jnp.bfloat16):
    values = scale * jax.random.normal(own_key, shape, jnp.float32)
    if cuts:
        values = values * steps_of(own_key, shape, cuts, -0.22, 0.18)
    return jnp.clip(values, -limit, limit).astype(kind)


def setup_inputs(seed: int = 0) -> dict:
    keys = jax.random.split(jax.random.key(seed), 10)
    return {
        "q_latent": draw_q_latent(jax.random.fold_in(keys[9], 71), 0),
        "kv_latent": draw_kv_latent(jax.random.fold_in(keys[9], 71), 0),
        "rope_key": draw_rope_key(jax.random.fold_in(keys[9], 71), 0),
        "w_query": noise(keys[3], (QR, H * (NOPE + ROPE)), QR ** -0.5, 0.25, ((1, 8),)),
        "w_keyval": noise(keys[4], (KR, H * (NOPE + VDIM)), KR ** -0.5, 0.25, ((1, 4),)),
        "w_out": noise(keys[5], (H * VDIM, D), (H * VDIM) ** -0.5, 0.125),
        "query_gain": jnp.clip(1.0 + 0.18 * jax.random.normal(keys[6], (QR,), jnp.float32), 0.099609375, 1.8984375).astype(jnp.bfloat16),
        "latent_gain": jnp.clip(1.0 + 0.18 * jax.random.normal(keys[7], (KR,), jnp.float32), 0.099609375, 1.8984375).astype(jnp.bfloat16),
        "out_gain": jnp.clip(1.0 + 0.18 * jax.random.normal(keys[8], (H * VDIM,), jnp.float32), 0.099609375, 1.8984375).astype(jnp.bfloat16),
    }


def normalize(row_values, gain_vector):
    widened = row_values.astype(jnp.float32)
    return widened * lax.rsqrt(lax.optimization_barrier(jnp.mean(widened * widened, axis=-1, keepdims=True)) + 1e-05) * gain_vector.astype(jnp.float32)

def angles_for(positions, rope_width):
    half_width = rope_width // 2
    inverse = 10000.0 ** (-jnp.arange(half_width, dtype=jnp.float32) / half_width)
    return positions.astype(jnp.float32)[:, None] * inverse[None, :]

def turn(vectors, angles):
    half_width = vectors.shape[-1] // 2
    cosine = jnp.cos(angles)
    sine_value = jnp.sin(angles)
    low_half = vectors[..., :half_width]
    high_half = vectors[..., half_width:]
    return jnp.concatenate([low_half * cosine - high_half * sine_value, high_half * cosine + low_half * sine_value], axis=-1)

def one_sequence(query_latent, kv_rows, rope_rows, w_query, w_keyval, w_out, query_gain, latent_gain, out_gain):
    length = query_latent.shape[0]
    positions = jnp.arange(length, dtype=jnp.int32)
    angles = angles_for(positions, ROPE)
    query_norm = normalize(query_latent, query_gain).astype(jnp.bfloat16)
    query_raw = jnp.dot(query_norm, w_query, preferred_element_type=jnp.float32).reshape(length, H, NOPE + ROPE)
    queries = jnp.concatenate([query_raw[..., :NOPE], turn(query_raw[..., NOPE:], angles[:, None, :])], axis=-1).astype(jnp.bfloat16)
    queries = lax.optimization_barrier(queries)
    latent_norm = normalize(kv_rows, latent_gain).astype(jnp.bfloat16)
    keyval = jnp.dot(latent_norm, w_keyval, preferred_element_type=jnp.float32).astype(jnp.bfloat16)
    keyval = lax.optimization_barrier(keyval).reshape(length, H, NOPE + VDIM)
    rope_turned = turn(rope_rows.astype(jnp.float32), angles).astype(jnp.bfloat16)
    rope_turned = lax.optimization_barrier(rope_turned)
    key_rows = jnp.concatenate([keyval[..., :NOPE], jnp.broadcast_to(rope_turned[:, None, :], (length, H, ROPE))], axis=-1)
    value_rows = keyval[..., NOPE:]
    block_rows = min(512, length)
    score_scale = (NOPE + ROPE) ** (-0.5)
    pieces = []
    for block_index in range(length // block_rows):
        block_start = block_index * block_rows
        block_stop = block_start + block_rows
        scores = jnp.einsum('qhd,khd->hqk', queries[block_start:block_stop].astype(jnp.float32), key_rows[:block_stop].astype(jnp.float32)) * score_scale
        allowed = jnp.arange(block_stop)[None, :] <= (block_start + jnp.arange(block_rows))[:, None]
        scores = jnp.where(allowed[None], scores, -jnp.inf)
        row_top = lax.optimization_barrier(jnp.max(scores, axis=-1, keepdims=True))
        exponent = jnp.exp(scores - row_top)
        row_total = lax.optimization_barrier(jnp.sum(exponent, axis=-1))
        weights = lax.optimization_barrier(exponent.astype(jnp.bfloat16))
        summed = jnp.einsum('hqk,khd->qhd', weights.astype(jnp.float32), value_rows[:block_stop].astype(jnp.float32))
        pieces.append((summed / jnp.transpose(row_total)[:, :, None]).astype(jnp.bfloat16))
    attended = lax.optimization_barrier(jnp.concatenate(pieces, axis=0)).reshape(length, H * VDIM)
    mixed_norm = normalize(attended, out_gain).astype(jnp.bfloat16)
    return jnp.dot(mixed_norm, w_out, preferred_element_type=jnp.float32).astype(jnp.bfloat16)

def reference(q_latent, kv_latent, rope_key, w_query, w_keyval, w_out, query_gain, latent_gain, out_gain):

    def per_sequence(inputs):
        return one_sequence(inputs[0], inputs[1], inputs[2], w_query, w_keyval, w_out, query_gain, latent_gain, out_gain)
    return lax.map(per_sequence, (q_latent, kv_latent, rope_key))
```

```python
import functools

import jax
import jax.numpy as jnp
from jax import lax
from jax.experimental import pallas as pl
from jax.experimental.pallas import tpu as pltpu
from jax.sharding import PartitionSpec as P

H = 16
NOPE = 128
ROPE = 64
VDIM = 128
HEAD = NOPE + ROPE
PAIR = 2
EPS = 1e-05
LOG2E = 1.4426950408889634
VMEM = pltpu.VMEM
SMEM = pltpu.SMEM


def normalize(row_values, gain_vector):
    widened = row_values.astype(jnp.float32)
    return (
        widened
        * lax.rsqrt(jnp.mean(widened * widened, axis=-1, keepdims=True) + EPS)
        * gain_vector.astype(jnp.float32)
    )


def angles_for(positions, rope_width):
    half_width = rope_width // 2
    inverse = 10000.0 ** (-jnp.arange(half_width, dtype=jnp.float32) / half_width)
    return positions.astype(jnp.float32)[:, None] * inverse[None, :]


def turn(vectors, angles):
    half_width = vectors.shape[-1] // 2
    cosine = jnp.cos(angles)
    sine_value = jnp.sin(angles)
    low_half = vectors[..., :half_width]
    high_half = vectors[..., half_width:]
    return jnp.concatenate(
        [low_half * cosine - high_half * sine_value, high_half * cosine + low_half * sine_value],
        axis=-1,
    )


def attend(query_head, keyval_head, rope_all):
    length = query_head.shape[0]
    local_heads = query_head.shape[1] // HEAD
    query_three = query_head.reshape(length, local_heads, HEAD)
    keyval_three = keyval_head.reshape(length, local_heads, NOPE + VDIM)
    block_rows = min(512, length)
    score_scale = HEAD ** (-0.5)
    pieces = []
    for block_index in range(length // block_rows):
        block_start = block_index * block_rows
        block_stop = block_start + block_rows
        query_block = query_three[block_start:block_stop]
        scores = jnp.einsum(
            "qhd,khd->hqk",
            query_block[..., :NOPE],
            keyval_three[:block_stop, :, :NOPE],
            preferred_element_type=jnp.float32,
        )
        scores = scores + jnp.einsum(
            "qhr,kr->hqk",
            query_block[..., NOPE:],
            rope_all[:block_stop],
            preferred_element_type=jnp.float32,
        )
        scores = scores * score_scale
        allowed = jnp.arange(block_stop)[None, :] <= (block_start + jnp.arange(block_rows))[:, None]
        scores = jnp.where(allowed[None], scores, -jnp.inf)
        row_top = jnp.max(scores, axis=-1, keepdims=True)
        exponent = jnp.exp(scores - row_top)
        row_total = jnp.sum(exponent, axis=-1)
        summed = jnp.einsum(
            "hqk,khd->qhd",
            exponent.astype(jnp.bfloat16),
            keyval_three[:block_stop, :, NOPE:],
            preferred_element_type=jnp.float32,
        )
        pieces.append((summed / jnp.transpose(row_total)[:, :, None]).astype(jnp.bfloat16))
    return jnp.concatenate(pieces, axis=0).reshape(length, local_heads * VDIM)


def general_plan(
    q_latent, kv_latent, rope_key, w_query, w_keyval, w_out, query_gain, latent_gain, out_gain
):
    tokens_here = q_latent.shape[1]
    offset = lax.axis_index("sp") * tokens_here
    positions = offset + jnp.arange(tokens_here, dtype=jnp.int32)
    angles = angles_for(positions, ROPE)
    query_norm = normalize(q_latent[0], query_gain).astype(jnp.bfloat16)
    query_raw = jnp.dot(
        query_norm,
        lax.all_gather(w_query, "dp", axis=1, tiled=True),
        preferred_element_type=jnp.float32,
    )
    query_raw = query_raw.reshape(tokens_here, H, HEAD)
    queries = jnp.concatenate(
        [query_raw[..., :NOPE], turn(query_raw[..., NOPE:], angles[:, None, :])], axis=-1
    )
    queries = queries.astype(jnp.bfloat16).reshape(tokens_here, H * HEAD)
    latent_norm = normalize(kv_latent[0], latent_gain).astype(jnp.bfloat16)
    rope_turned = turn(rope_key[0].astype(jnp.float32), angles).astype(jnp.bfloat16)
    query_head = lax.all_to_all(queries, "sp", split_axis=1, concat_axis=0, tiled=True)
    latent_all, rope_all = (
        lax.all_gather(latent_norm, "sp", axis=0, tiled=True),
        lax.all_gather(rope_turned, "sp", axis=0, tiled=True),
    )
    keyval_head = jnp.dot(latent_all, w_keyval, preferred_element_type=jnp.float32).astype(
        jnp.bfloat16
    )
    attended = attend(query_head, keyval_head, rope_all)
    returned = lax.all_to_all(attended, "sp", split_axis=0, concat_axis=1, tiled=True)
    mixed_norm = normalize(returned, out_gain).astype(jnp.bfloat16)
    result = jnp.dot(mixed_norm, w_out, preferred_element_type=jnp.float32).astype(jnp.bfloat16)
    return result[None]


def vmem_spec():
    return pl.BlockSpec(memory_space=VMEM)


def smem_spec():
    return pl.BlockSpec(memory_space=SMEM)


def call(kernel, out_shape, n_smem, n_vmem, name, limit=24, scratch=(), specs=None):
    n_out = len(out_shape)
    return pl.pallas_call(
        kernel,
        out_shape=out_shape,
        in_specs=[smem_spec()] * n_smem + (specs or [vmem_spec()] * n_vmem),
        out_specs=[vmem_spec()] * n_out,
        scratch_shapes=list(scratch),
        compiler_params=pltpu.CompilerParams(vmem_limit_bytes=limit * 1024 * 1024),
        name=name,
    )


def norm_rows(values, gain):
    wide = values.astype(jnp.float32)
    mean = jnp.mean(wide * wide, axis=-1, keepdims=True)
    return wide * lax.rsqrt(mean + EPS) * gain.astype(jnp.float32)


def frequency(index, half):
    return jnp.exp2(index.astype(jnp.float32) * (-13.287712379549449 / half))


def prologue_kernel(s_ref, q_ref, kv_ref, rope_ref, qg_ref, lg_ref, out_ref):
    rows, width = q_ref.shape
    out_ref[:, :width] = norm_rows(q_ref[...], qg_ref[...]).astype(jnp.bfloat16)
    out_ref[:, width : 2 * width] = norm_rows(kv_ref[...], lg_ref[...]).astype(jnp.bfloat16)
    half = rope_ref.shape[0] // 2
    place = lax.broadcasted_iota(jnp.int32, (half, rows), 1) + s_ref[0] * rows
    angle = place.astype(jnp.float32) * frequency(
        lax.broadcasted_iota(jnp.int32, (half, rows), 0), half
    )
    cosine = jnp.cos(angle)
    sine = jnp.sin(angle)
    low = rope_ref[:half, :].astype(jnp.float32)
    high = rope_ref[half:, :].astype(jnp.float32)
    first = low * cosine - high * sine
    second = high * cosine + low * sine
    turned = jnp.concatenate([first, second, first, second], axis=0)
    out_ref[:, 2 * width :] = turned.T.astype(jnp.bfloat16)


def keyval_kernel(s_ref, *refs, blocks, width):
    packs = refs[: len(blocks)]
    w_ref, kv_ref, cos_ref, sin_ref = refs[len(blocks) :]
    rows = packs[0].shape[0]
    pieces = kv_ref.shape[0]
    cols = kv_ref.shape[2]
    latent = jnp.concatenate([p[:, width : 2 * width] for p in packs], axis=0)
    for piece in range(pieces):
        kv_ref[piece] = jnp.dot(
            latent,
            w_ref[:, piece * cols : (piece + 1) * cols],
            preferred_element_type=jnp.float32,
        ).astype(jnp.bfloat16)
    half = ROPE // 2
    lane = lax.broadcasted_iota(jnp.int32, (rows, 2 * ROPE), 1)
    freq = frequency(lane % half, half)
    sign = jnp.where(lane % ROPE < half, -1.0, 1.0)
    for i, flip in enumerate(blocks):
        start = (s_ref[0] ^ flip) * rows
        place = lax.broadcasted_iota(jnp.int32, (rows, 2 * ROPE), 0) + start
        angle = place.astype(jnp.float32) * freq
        cos_ref[i * rows : (i + 1) * rows, :] = jnp.cos(angle)
        sin_ref[i * rows : (i + 1) * rows, :] = jnp.sin(angle) * sign


def attend_kernel(s_ref, *refs, blocks, width, shift, pieces):
    n = len(blocks)
    packs = refs[:n]
    w_refs = refs[n : n + 2]
    kv_ref, cos_ref, sin_ref = refs[n + 2 : n + 5]
    outs = refs[n + 5 : n + 5 + n]
    rows = packs[0].shape[0]
    length = rows * n
    piece = lax.rem(s_ref[1] + shift, pieces)
    half = ROPE // 2
    query_norm = jnp.concatenate([p[:, :width] for p in packs], axis=0)
    rope = jnp.concatenate([p[:, 2 * width :] for p in packs], axis=0)
    split = w_refs[0].shape[0]
    raw = jnp.dot(query_norm[:, :split], w_refs[0][...], preferred_element_type=jnp.float32)
    raw += jnp.dot(query_norm[:, split:], w_refs[1][...], preferred_element_type=jnp.float32)
    lane = lax.broadcasted_iota(jnp.int32, (length, 2 * ROPE), 1)
    one = raw[:, NOPE : 2 * NOPE]
    two = raw[:, 2 * NOPE :]
    is_low = lane < ROPE
    plain = [
        raw[:, :NOPE],
        jnp.where(is_low, pltpu.roll(one, ROPE, 1), pltpu.roll(two, ROPE, 1)),
    ]
    rotary = jnp.where(is_low, one, two)
    swapped = jnp.where(
        lane % ROPE < half, pltpu.roll(rotary, 2 * ROPE - half, 1), pltpu.roll(rotary, half, 1)
    )
    rotary = rotary * cos_ref[...] + swapped * sin_ref[...]
    keys_at = jnp.concatenate(
        [
            lax.broadcasted_iota(jnp.int32, (rows, rows), 1) + (s_ref[0] ^ flip) * rows
            for flip in blocks
        ],
        axis=1,
    )
    for head in range(PAIR):
        keep = is_low if head == 0 else jnp.logical_not(is_low)
        query = jnp.concatenate(
            [plain[head], jnp.where(keep, rotary, 0.0)], axis=1
        ).astype(jnp.bfloat16)
        base = head * (NOPE + VDIM)
        key = jnp.concatenate([kv_ref[piece, :, base : base + NOPE], rope], axis=1)
        value = kv_ref[piece, :, base + NOPE : base + NOPE + VDIM]
        for i, flip in enumerate(blocks):
            scores = lax.dot_general(
                query[i * rows : (i + 1) * rows],
                key,
                (((1,), (1,)), ((), ())),
                preferred_element_type=jnp.float32,
            )
            place = lax.broadcasted_iota(jnp.int32, (rows, length), 0) + (s_ref[0] ^ flip) * rows
            scores = jnp.where(keys_at <= place, scores, -jnp.inf)
            top = jnp.max(scores, axis=-1, keepdims=True)
            weight = jnp.exp2((scores - top) * (HEAD ** (-0.5) * LOG2E))
            total = jnp.sum(weight, axis=-1, keepdims=True)
            summed = jnp.dot(
                weight.astype(jnp.bfloat16), value, preferred_element_type=jnp.float32
            )
            outs[i][:, head * VDIM : (head + 1) * VDIM] = (summed / total).astype(jnp.bfloat16)


def project_kernel(s_ref, *refs, blocks, shift, pieces, first, last):
    n = len(blocks)
    parts = refs[:n]
    gain_ref, w_ref = refs[n : n + 2]
    rest = refs[n + 2 :]
    piece = lax.rem(s_ref[1] + shift, pieces)
    total = None
    squares = None
    for part, flip in zip(parts, blocks):
        which = (s_ref[0] ^ flip) * pieces + piece
        wide = part[...].astype(jnp.float32)
        square = jnp.sum(wide * wide, axis=-1, keepdims=True)
        scaled = (wide * gain_ref[which].astype(jnp.float32)).astype(jnp.bfloat16)
        done = jnp.dot(scaled, w_ref[which], preferred_element_type=jnp.float32)
        total = done if total is None else total + done
        squares = square if squares is None else squares + square
    if not first:
        old_ref, old_sq, rest = rest[0], rest[1], rest[2:]
        total = total + old_ref[...]
        squares = squares + old_sq[:, :1]
    if last:
        factor = lax.rsqrt(squares * (1.0 / (gain_ref.shape[0] * gain_ref.shape[2])) + EPS)
        rest[0][...] = (total * factor).astype(jnp.bfloat16)
    else:
        rest[0][...] = total
        rest[1][...] = jnp.broadcast_to(squares, rest[1].shape)


def paired_plan(
    q_latent, kv_latent, rope_key, w_query, w_keyval, w_out, query_gain, latent_gain, out_gain, sp, dp
):
    rows = q_latent.shape[1]
    width = q_latent.shape[2]
    length = rows * sp
    pieces = dp // sp
    sp_at = lax.axis_index("sp")
    dp_at = lax.axis_index("dp")
    where = jnp.stack([sp_at, dp_at % pieces]).astype(jnp.int32)
    steps = []
    bit = sp // 2
    while bit:
        steps.append(bit)
        bit //= 2
    blocks = [0]
    for step in steps:
        blocks = blocks + [b ^ step for b in blocks]

    def swap(value, flip):
        return lax.ppermute(value, "sp", [(i, i ^ flip) for i in range(sp)])

    def fetch(value, turn_by, parity):
        pairs = []
        for s in range(sp):
            for zone in range(sp):
                for x in range(pieces):
                    at = (zone + parity) % 2
                    source = (at * (sp // 2) + zone // 2, s * pieces + (x + turn_by) % pieces)
                    pairs.append((source[0] * dp + source[1], s * dp + zone * pieces + x))
        return lax.ppermute(value, ("sp", "dp"), pairs)

    cut = w_query.shape[0] // 2
    halves = [w_query[:cut], w_query[cut:]]
    weights = [[fetch(halves[h], j, j + h) for h in range(2)] for j in range(pieces)]

    pack = call(
        prologue_kernel,
        [jax.ShapeDtypeStruct((rows, 2 * width + 2 * ROPE), jnp.bfloat16)],
        1,
        5,
        "prologue",
    )(where, q_latent[0], kv_latent[0], rope_key[0].T, query_gain[None], latent_gain[None])[0]
    packs = [pack]
    for step in steps:
        packs = packs + [swap(p, step) for p in packs]

    group = PAIR * (NOPE + VDIM)
    keyval, cosine, sine = call(
        functools.partial(keyval_kernel, blocks=blocks, width=width),
        [
            jax.ShapeDtypeStruct((pieces, length, group), jnp.bfloat16),
            jax.ShapeDtypeStruct((length, 2 * ROPE), jnp.float32),
            jax.ShapeDtypeStruct((length, 2 * ROPE), jnp.float32),
        ],
        1,
        sp + 1,
        "keyval",
    )(where, *packs, w_keyval)

    w_out_group = w_out.reshape(sp * pieces, PAIR * VDIM, w_out.shape[1])
    gain_group = out_gain.reshape(sp * pieces, 1, PAIR * VDIM)
    state = []
    for j in range(pieces):
        outs = call(
            functools.partial(attend_kernel, blocks=blocks, width=width, shift=j, pieces=pieces),
            [jax.ShapeDtypeStruct((rows, PAIR * VDIM), jnp.bfloat16)] * sp,
            1,
            sp + 5,
            f"attend{j}",
        )(where, *packs, *weights[j], keyval, cosine, sine)
        back = [o if flip == 0 else swap(o, flip) for o, flip in zip(outs, blocks)]
        last = j == pieces - 1
        shapes = (
            [jax.ShapeDtypeStruct((rows, w_out.shape[1]), jnp.bfloat16)]
            if last
            else [
                jax.ShapeDtypeStruct((rows, w_out.shape[1]), jnp.float32),
                jax.ShapeDtypeStruct((rows, 128), jnp.float32),
            ]
        )
        state = call(
            functools.partial(
                project_kernel, blocks=blocks, shift=j, pieces=pieces, first=j == 0, last=last
            ),
            shapes,
            1,
            sp + 2 + len(state),
            f"project{j}",
        )(where, *back, gain_group, w_out_group, *state)
    return state[0][None]


def solution(mesh):
    sp = mesh.shape["sp"]
    dp = mesh.shape["dp"]
    in_specs = (
        P("dp", "sp", None),
        P("dp", "sp", None),
        P("dp", "sp", None),
        P(None, "dp"),
        P(None, "sp"),
        P(),
        P(),
        P(),
        P(),
    )
    out_specs = P("dp", "sp", None)

    def per_device(*arrays):
        q_latent, w_query = arrays[0], arrays[3]
        paired = (
            sp & (sp - 1) == 0
            and sp > 1
            and dp % sp == 0
            and w_query.shape[1] == PAIR * HEAD
            and q_latent.shape[1] % 128 == 0
            and q_latent.shape[1] * sp <= 1024
        )
        if paired:
            return paired_plan(*arrays, sp=sp, dp=dp)
        return general_plan(*arrays)

    return jax.shard_map(
        per_device, mesh=mesh, in_specs=in_specs, out_specs=out_specs, check_vma=False
    )
```
